256 devices in a mesh: grp: 2 (over z), sp: 16 (over y, core), tp: 8 (over x).
Axes of the slice: x: 8, y: 8, z: 2, core: 2. Of those that a mesh axis runs over, the one named last changes fastest.
The devices are a block of a 8x8x16 slice.
Arguments:
- layer_input: bfloat16 [32, 4096, 2048], P(('grp', 'tp'), 'sp'), parts along dimension 0, may hold values from -6 to 6
- norm_gain: bfloat16 [2048], replicated, may hold values from 0.099609375 to 1.8984375
- key_weight: bfloat16 [2048, 1024], replicated, may hold values from -0.125 to 0.125
- value_weight: bfloat16 [2048, 1024], replicated, may hold values from -0.125 to 0.125
- input_gate_weight: bfloat16 [2048, 8], replicated, may hold values from -0.125 to 0.125
- forget_gate_weight: bfloat16 [2048, 8], replicated, may hold values from -0.125 to 0.125
- conv_weight: float32 [4, 1024], replicated, may hold values from -3 to 3
- input_shift: float32 [32, 8, 4096], P(('grp', 'sp'), 'tp'), parts along dimension 0, may hold values from -4 to 302
- forget_shift: float32 [32, 8, 4096], P(('grp', 'sp'), 'tp'), parts along dimension 0, may hold values from 0 to 10.1
- new_query: bfloat16 [32, 8, 128], P(('grp', 'sp'), 'tp'), parts along dimension 0, may hold values from 0.1 to 2
- new_key: bfloat16 [32, 8, 128], P(('grp', 'sp'), 'tp'), parts along dimension 0, may hold values from -6 to 6
- new_value: bfloat16 [32, 8, 128], P(('grp', 'sp'), 'tp'), parts along dimension 0, may hold values from -6 to 6
- new_input: float32 [32, 8], P(('grp', 'sp'), 'tp'), parts along dimension 0, may hold values from 2 to 6
- new_forget: float32 [32, 8], P(('grp', 'sp'), 'tp'), parts along dimension 0, may hold values from -1 to 3
Outputs:
- key_cache: bfloat16 [32, 8, 4096, 128], P(('grp', 'sp'), 'tp'), parts along dimension 0
- value_cache: bfloat16 [32, 8, 4096, 128], P(('grp', 'sp'), 'tp'), parts along dimension 0
- weight_cache: float32 [32, 8, 4096], P(('grp', 'sp'), 'tp'), parts along dimension 0
- first_read: bfloat16 [32, 8, 128], P(('grp', 'sp'), 'tp'), parts along dimension 0
The draws below stay inside these ranges and needn't reach their ends.
There are 2 independent parts, one for each index of `grp`. The reference program is written for one: setup_inputs(seed, part) draws one part's arguments, and reference() takes and returns one part's arrays. A program takes and returns all parts, laid end to end along the dimension named above; an argument that names none is the same for every part. Nothing has to cross between parts.
All inputs are finite; a program needn't handle non-finite values.
Results may differ from the reference program's by a relative error of at most 0.012.
Values may be sent and summed in bfloat16 or wider, within the bound.
No kernel may reach another device: no remote copies, remote signals or barrier semaphores. Data moves between devices by JAX's collectives and lax.ppermute only.
A program may use at most 64 MiB of HBM per device.

```python
import jax
import jax.numpy as jnp
from jax import lax

D = 2048
HEADS = 8
DK = 128
CONV = 4
POS_DEV = 256
SEQS = 16
LENGTH = 4096


def draw_input_shift(key, part):
    subkeys = jax.random.split(key, 1)
    return jnp.clip(jax.random.normal(subkeys[0], (SEQS, HEADS, LENGTH), jnp.float32), -4.0, 4.0)


def draw_forget_shift(key, part):
    subkeys = jax.random.split(key, 5)
    slow_share = 0.5
    slower = jax.random.uniform(subkeys[0], (SEQS, HEADS, 1), jnp.float32) < slow_share
    slow_level = jnp.log(jnp.float32(LENGTH))
    fast_level = jax.random.uniform(subkeys[1], (SEQS, HEADS, 1), jnp.float32, 3.4, 4.6)
    block_list = LENGTH // POS_DEV
    factor = jax.random.uniform(subkeys[2], (SEQS, HEADS, block_list, 1), jnp.float32, -0.7, 0.7)
    factor = jnp.broadcast_to(factor, (SEQS, HEADS, block_list, POS_DEV)).reshape(SEQS, HEADS, LENGTH)
    level_values = jnp.where(slower, slow_level, fast_level) + factor
    targets = jax.random.randint(subkeys[3], (SEQS, HEADS, 4), 0, LENGTH)
    level_heights = jax.random.uniform(subkeys[4], (SEQS, HEADS, 4), jnp.float32, 0.0, 1.4)
    places = jnp.arange(LENGTH)
    match_hits = places[None, None, None, :] == targets[:, :, :, None]
    surge_counts = jnp.any(match_hits, axis=2)
    surge_level = jnp.max(jnp.where(match_hits, level_heights[:, :, :, None], -1.0), axis=2)
    return jnp.where(surge_counts, surge_level, level_values)


def draw_new_query(key, part):
    subkeys = jax.random.split(jax.random.fold_in(key, 17), 2)
    drawn = 1.0 + 0.5 * jax.random.normal(subkeys[1], (SEQS, HEADS, DK), jnp.float32)
    return jnp.clip(drawn, 0.1, 2.0).astype(jnp.bfloat16)


def shard_levels(own_key, extent, cuts, least, high):
    level, own = 1.0, jax.random.fold_in(own_key, 6)
    for axis_at, blocks in cuts:
        heights = jnp.exp(jax.random.uniform(jax.random.fold_in(own, axis_at), (blocks,), jnp.float32, least / len(cuts), high / len(cuts)))
        level = level * jnp.repeat(heights, extent[axis_at] // blocks).reshape([-1 if axis == axis_at else 1 for axis in range(len(extent))])
    return level


def bell_draw(own_key, extent, deviation, bound, pieces=(), held_as=jnp.bfloat16):
    values = jax.random.normal(own_key, extent, jnp.float32) * deviation
    if len(pieces) > 0:
        values = shard_levels(own_key, extent, pieces, -0.22, 0.18) * values
    return jnp.clip(values, min=-bound, max=bound).astype(held_as)


def setup_inputs(seed: int = 0, part: int = 0) -> dict:
    key_list = jax.random.split(jax.random.key(seed), 15)
    part_keys = jax.random.split(jax.random.fold_in(key_list[14], part), 15)
    return {
        "layer_input": bell_draw(part_keys[0], (SEQS, LENGTH, D), 1.0, 6.0, ((0, 8), (1, 16))),
        "norm_gain": jnp.clip(1.0 + 0.18 * jax.random.normal(key_list[1], (D,), jnp.float32), 0.099609375, 1.8984375).astype(jnp.bfloat16),
        "key_weight": bell_draw(key_list[2], (D, HEADS * DK), D ** -0.5, 0.125),
        "value_weight": bell_draw(key_list[3], (D, HEADS * DK), D ** -0.5, 0.125),
        "input_gate_weight": bell_draw(key_list[4], (D, HEADS), D ** -0.5, 0.125),
        "forget_gate_weight": bell_draw(key_list[5], (D, HEADS), D ** -0.5, 0.125),
        "conv_weight": bell_draw(key_list[6], (CONV, HEADS * DK), 0.5, 3.0, (), jnp.float32),
        "input_shift": draw_input_shift(jax.random.fold_in(jax.random.fold_in(key_list[14], part), 71), part),
        "forget_shift": draw_forget_shift(jax.random.fold_in(jax.random.fold_in(key_list[14], part), 71), part),
        "new_query": draw_new_query(jax.random.fold_in(jax.random.fold_in(key_list[14], part), 71), part),
        "new_key": bell_draw(part_keys[10], (SEQS, HEADS, DK), 1.0, 6.0, ((0, 16), (1, 8))),
        "new_value": bell_draw(part_keys[11], (SEQS, HEADS, DK), 1.0, 6.0, ((0, 16), (1, 8))),
        "new_input": jnp.clip(2.0 + 4.0 * jax.random.uniform(part_keys[12], (SEQS, HEADS), jnp.float32) ** shard_levels(part_keys[12], (SEQS, HEADS), ((0, 16), (1, 8)), -0.2, 0.2), 2.0, 6.0),
        "new_forget": jnp.clip(-1.0 + 4.0 * jax.random.uniform(part_keys[13], (SEQS, HEADS), jnp.float32) ** shard_levels(part_keys[13], (SEQS, HEADS), ((0, 16), (1, 8)), -0.2, 0.2), -1.0, 3.0),
    }


epsilon = 1e-06

def one_sequence(token_rows, norm_gain, key_weight, value_weight, input_gate_weight, forget_gate_weight, conv_weight):
    widened = token_rows.astype(jnp.float32)
    normed = (widened * lax.rsqrt(lax.optimization_barrier(jnp.mean(widened * widened, axis=-1, keepdims=True)) + epsilon) * norm_gain.astype(jnp.float32)).astype(jnp.bfloat16)
    key_linear = jnp.dot(normed, key_weight, preferred_element_type=jnp.float32).astype(jnp.bfloat16)
    values = jnp.dot(normed, value_weight, preferred_element_type=jnp.float32).astype(jnp.bfloat16)
    input_linear = jnp.dot(normed, input_gate_weight, preferred_element_type=jnp.float32).astype(jnp.bfloat16)
    forget_linear = jnp.dot(normed, forget_gate_weight, preferred_element_type=jnp.float32).astype(jnp.bfloat16)
    padded = jnp.pad(key_linear.astype(jnp.float32), ((CONV - 1, 0), (0, 0)))
    summed = padded[0:LENGTH] * conv_weight[0]
    for offset in range(1, CONV):
        summed = summed + padded[offset:offset + LENGTH] * conv_weight[offset]
    keys = jax.nn.silu(summed).astype(jnp.bfloat16)
    keys = keys.reshape(LENGTH, HEADS, DK).transpose(1, 0, 2)
    values = values.reshape(LENGTH, HEADS, DK).transpose(1, 0, 2)
    return (keys, values, input_linear.T, forget_linear.T)

def read_cache(keys, values, input_linear, forget_linear, input_shift, forget_shift, new_query, new_key, new_value, new_input, new_forget):
    scaling = DK ** (-0.5)
    log_forget = jax.nn.log_sigmoid(forget_linear.astype(jnp.float32) + forget_shift)
    suffix = lax.cumsum(log_forget, axis=2, reverse=True) - log_forget
    new_decay = jax.nn.log_sigmoid(new_forget)
    log_weight = input_linear.astype(jnp.float32) + input_shift + suffix + new_decay[:, :, None]
    largest = jnp.maximum(lax.optimization_barrier(jnp.max(log_weight, axis=2)), new_input)
    weight_cache = jnp.exp(log_weight - largest[:, :, None])
    new_weight = jnp.exp(new_input - largest)
    matched = jnp.einsum('bhlk,bhk->bhl', keys.astype(jnp.float32), new_query.astype(jnp.float32))
    scores = (weight_cache * matched * scaling).astype(jnp.bfloat16)
    fresh_match = lax.optimization_barrier(jnp.sum(new_key.astype(jnp.float32) * new_query.astype(jnp.float32), axis=2))
    new_score = (new_weight * fresh_match * scaling).astype(jnp.bfloat16)
    denominator = lax.optimization_barrier(jnp.sum(scores.astype(jnp.float32), axis=2)) + new_score.astype(jnp.float32)
    numerator = jnp.einsum('bhl,bhlk->bhk', scores.astype(jnp.float32), values.astype(jnp.float32))
    numerator = numerator + new_score.astype(jnp.float32)[:, :, None] * new_value.astype(jnp.float32)
    first_read = (numerator / jnp.maximum(jnp.abs(denominator), 1.0)[:, :, None]).astype(jnp.bfloat16)
    return (weight_cache, first_read)

def reference(layer_input, norm_gain, key_weight, value_weight, input_gate_weight, forget_gate_weight, conv_weight, input_shift, forget_shift, new_query, new_key, new_value, new_input, new_forget):

    def project(token_rows):
        return one_sequence(token_rows, norm_gain, key_weight, value_weight, input_gate_weight, forget_gate_weight, conv_weight)
    keys, values, input_linear, forget_linear = lax.map(project, layer_input)
    weight_cache, first_read = read_cache(keys, values, input_linear, forget_linear, input_shift, forget_shift, new_query, new_key, new_value, new_input, new_forget)
    return (keys, values, weight_cache, first_read)
```

```python
import jax
import jax.numpy as jnp
from jax import lax
from jax.sharding import PartitionSpec as P

HEADS = 8
DK = 128
CONV = 4


epsilon = 1e-06


def normalise(token_rows, norm_gain):
    widened = token_rows.astype(jnp.float32)
    return (
        widened
        * lax.rsqrt(jnp.mean(widened * widened, axis=-1, keepdims=True) + epsilon)
        * norm_gain.astype(jnp.float32)
    ).astype(jnp.bfloat16)


def project(normed, weight):
    matrix = weight.reshape(weight.shape[0], HEADS, DK)
    return jnp.einsum(
        "apd,dhk->hapk", normed, matrix, preferred_element_type=jnp.float32
    ).astype(jnp.bfloat16)


def gate(normed, weight):
    linear = jnp.einsum("apd,dh->hap", normed, weight, preferred_element_type=jnp.float32)
    return linear.astype(jnp.bfloat16)


def convolve(key_linear, tap_weight):
    length = key_linear.shape[0]
    extended = jnp.pad(key_linear.astype(jnp.float32), ((CONV - 1, 0), (0, 0)))
    summed = extended[0:length] * tap_weight[0]
    for offset in range(1, CONV):
        summed = summed + extended[offset : offset + length] * tap_weight[offset]
    return jax.nn.silu(summed).astype(jnp.bfloat16)


def read_cache(
    keys,
    values,
    input_linear,
    forget_linear,
    input_shift,
    forget_shift,
    new_query,
    new_key,
    new_value,
    new_input,
    new_forget,
):
    scaling = DK ** (-0.5)
    log_forget = jax.nn.log_sigmoid(forget_linear.astype(jnp.float32) + forget_shift)
    suffix = lax.cumsum(log_forget, axis=2, reverse=True) - log_forget
    new_decay = jax.nn.log_sigmoid(new_forget)
    log_weight = input_linear.astype(jnp.float32) + input_shift + suffix + new_decay[:, :, None]
    largest = jnp.maximum(jnp.max(log_weight, axis=2), new_input)
    weight_cache = jnp.exp(log_weight - largest[:, :, None])
    new_weight = jnp.exp(new_input - largest)
    matched = jnp.einsum("bhlk,bhk->bhl", keys, new_query, preferred_element_type=jnp.float32)
    scores = (weight_cache * matched * scaling).astype(jnp.bfloat16)
    fresh_match = jnp.sum(new_key.astype(jnp.float32) * new_query.astype(jnp.float32), axis=2)
    new_score = (new_weight * fresh_match * scaling).astype(jnp.bfloat16)
    denominator = jnp.sum(scores.astype(jnp.float32), axis=2) + new_score.astype(jnp.float32)
    numerator = jnp.einsum("bhl,bhlk->bhk", scores, values, preferred_element_type=jnp.float32)
    numerator = numerator + new_score.astype(jnp.float32)[:, :, None] * new_value.astype(
        jnp.float32
    )
    first_read = (numerator / jnp.maximum(jnp.abs(denominator), 1.0)[:, :, None]).astype(
        jnp.bfloat16
    )
    return (weight_cache, first_read)


def shards(
    layer_input,
    norm_gain,
    key_weight,
    value_weight,
    input_gate_weight,
    forget_gate_weight,
    conv_weight,
    input_shift,
    forget_shift,
    new_query,
    new_key,
    new_value,
    new_input,
    new_forget,
):
    seqs, rows, _ = layer_input.shape
    lines = rows // DK
    normed = normalise(layer_input, norm_gain)
    gates = jnp.stack(
        [gate(normed, input_gate_weight), gate(normed, forget_gate_weight)], axis=2
    ).reshape(HEADS, seqs, 2 * lines, DK)
    gates = jnp.pad(gates, ((0, 0), (0, 0), (0, 8 - 2 * lines), (0, 0)))
    block = jnp.concatenate(
        [project(normed, key_weight), project(normed, value_weight), gates], axis=2
    )
    by_head = lax.all_to_all(block, "tp", split_axis=0, concat_axis=0, tiled=True)
    by_head = by_head.reshape(-1, *block.shape[2:])
    mine = lax.all_to_all(by_head, "sp", split_axis=0, concat_axis=0, tiled=True)
    blocks = mine.shape[0]
    length = blocks * rows
    key_linear = mine[:, :rows].reshape(length, DK)
    values = mine[:, rows : 2 * rows].reshape(1, 1, length, DK)
    input_linear = mine[:, 2 * rows : 2 * rows + lines].reshape(1, 1, length)
    forget_linear = mine[:, 2 * rows + lines : 2 * rows + 2 * lines].reshape(1, 1, length)
    head = lax.axis_index("tp")
    tap_weight = lax.dynamic_slice(conv_weight, (0, head * DK), (CONV, DK))
    keys = convolve(key_linear, tap_weight).reshape(1, 1, length, DK)
    weight_cache, first_read = read_cache(
        keys,
        values,
        input_linear,
        forget_linear,
        input_shift,
        forget_shift,
        new_query,
        new_key,
        new_value,
        new_input,
        new_forget,
    )
    return (keys, values, weight_cache, first_read)


def solution(mesh):
    in_specs = (
        P(("grp", "tp"), "sp", None),
        P(),
        P(),
        P(),
        P(),
        P(),
        P(),
        P(("grp", "sp"), "tp", None),
        P(("grp", "sp"), "tp", None),
        P(("grp", "sp"), "tp", None),
        P(("grp", "sp"), "tp", None),
        P(("grp", "sp"), "tp", None),
        P(("grp", "sp"), "tp"),
        P(("grp", "sp"), "tp"),
    )
    out_specs = (
        P(("grp", "sp"), "tp", None, None),
        P(("grp", "sp"), "tp", None, None),
        P(("grp", "sp"), "tp", None),
        P(("grp", "sp"), "tp", None),
    )
    return jax.shard_map(shards, mesh=mesh, in_specs=in_specs, out_specs=out_specs, check_vma=False)
```

```python
import jax
import jax.numpy as jnp
from jax import lax
from jax.sharding import PartitionSpec as P


HEADS = 8
DK = 128
CONV = 4


epsilon = 1e-06


def normalise(token_rows, norm_gain):
    widened = token_rows.astype(jnp.float32)
    return (
        widened
        * lax.rsqrt(jnp.mean(widened * widened, axis=-1, keepdims=True) + epsilon)
        * norm_gain.astype(jnp.float32)
    ).astype(jnp.bfloat16)


def project(normed, weight):
    matrix = weight.reshape(weight.shape[0], HEADS, DK)
    return jnp.einsum(
        "pd,dhk->hpk", normed, matrix, preferred_element_type=jnp.float32
    ).astype(jnp.bfloat16)


def gate(normed, weight):
    linear = jnp.einsum("pd,dh->hp", normed, weight, preferred_element_type=jnp.float32)
    return linear.astype(jnp.bfloat16)


def convolve(key_linear, tap_weight):
    length = key_linear.shape[0]
    extended = jnp.pad(key_linear.astype(jnp.float32), ((CONV - 1, 0), (0, 0)))
    summed = extended[0:length] * tap_weight[0]
    for offset in range(1, CONV):
        summed = summed + extended[offset : offset + length] * tap_weight[offset]
    return jax.nn.silu(summed).astype(jnp.bfloat16)


def read_cache(
    keys,
    values,
    input_linear,
    forget_linear,
    input_shift,
    forget_shift,
    new_query,
    new_key,
    new_value,
    new_input,
    new_forget,
):
    scaling = DK ** (-0.5)
    log_forget = jax.nn.log_sigmoid(forget_linear.astype(jnp.float32) + forget_shift)
    suffix = lax.cumsum(log_forget, axis=2, reverse=True) - log_forget
    new_decay = jax.nn.log_sigmoid(new_forget)
    log_weight = input_linear.astype(jnp.float32) + input_shift + suffix + new_decay[:, :, None]
    largest = jnp.maximum(jnp.max(log_weight, axis=2), new_input)
    weight_cache = jnp.exp(log_weight - largest[:, :, None])
    new_weight = jnp.exp(new_input - largest)
    matched = jnp.einsum("bhlk,bhk->bhl", keys, new_query, preferred_element_type=jnp.float32)
    scores = (weight_cache * matched * scaling).astype(jnp.bfloat16)
    fresh_match = jnp.sum(new_key.astype(jnp.float32) * new_query.astype(jnp.float32), axis=2)
    new_score = (new_weight * fresh_match * scaling).astype(jnp.bfloat16)
    denominator = jnp.sum(scores.astype(jnp.float32), axis=2) + new_score.astype(jnp.float32)
    numerator = jnp.einsum("bhl,bhlk->bhk", scores, values, preferred_element_type=jnp.float32)
    numerator = numerator + new_score.astype(jnp.float32)[:, :, None] * new_value.astype(
        jnp.float32
    )
    first_read = (numerator / jnp.maximum(jnp.abs(denominator), 1.0)[:, :, None]).astype(
        jnp.bfloat16
    )
    return (weight_cache, first_read)


def gather_sequence(layer_input):
    pair, rows, width = layer_input.shape
    core = lax.axis_index("sp") % pair
    own = lax.dynamic_index_in_dim(layer_input, core, 0, keepdims=False)
    other = lax.dynamic_index_in_dim(layer_input, 1 - core, 0, keepdims=False)
    route = [(i, i ^ 1) for i in range(lax.axis_size("sp"))]
    got = lax.ppermute(other, "sp", route)
    first = core == 0
    return jnp.stack([jnp.where(first, own, got), jnp.where(first, got, own)]).reshape(
        pair * rows, width
    )


def rotate(block):
    ring = lax.axis_size("tp")
    here = lax.axis_index("tp")
    got = []
    for step in range(ring):
        mine = lax.dynamic_index_in_dim(block, (here + step) % ring, 0, keepdims=False)
        if step:
            route = [(i, (i + step) % ring) for i in range(ring)]
            mine = lax.ppermute(mine, "tp", route)
        got.append(mine)
    return jnp.stack(got)


def spread(stack):
    ring, chips = lax.axis_size("sp"), stack.shape[0]
    pair = ring // chips
    column, chip = lax.axis_index("tp"), lax.axis_index("sp") // pair
    whole = jnp.zeros_like(stack)
    for step in range(chips):
        target = (chip + step) % chips
        mine = lax.dynamic_index_in_dim(stack, (column - target) % chips, 0, keepdims=False)
        if step:
            route = [(i, (i // pair + step) % chips * pair + i % pair) for i in range(ring)]
            mine = lax.ppermute(mine, "sp", route)
        whole = lax.dynamic_update_index_in_dim(whole, mine, (chip - step) % chips, 0)
    return whole


def layer(
    layer_input,
    norm_gain,
    key_weight,
    value_weight,
    input_gate_weight,
    forget_gate_weight,
    conv_weight,
    input_shift,
    forget_shift,
    new_query,
    new_key,
    new_value,
    new_input,
    new_forget,
):
    normed = normalise(gather_sequence(layer_input), norm_gain)
    rows = normed.shape[0]
    lines = rows // DK
    gates = jnp.stack([gate(normed, input_gate_weight), gate(normed, forget_gate_weight)], axis=1)
    gates = gates.reshape(HEADS, 2 * lines, DK)
    key_block = jnp.concatenate([project(normed, key_weight), gates], axis=1)
    normed, key_block = lax.optimization_barrier((normed, key_block))
    value_block = project(normed, value_weight)
    mine = spread(rotate(key_block))
    values = spread(rotate(value_block))
    length = mine.shape[0] * rows
    key_linear = mine[:, :rows].reshape(length, DK)
    values = values.reshape(1, 1, length, DK)
    input_linear = mine[:, rows : rows + lines].reshape(1, 1, length)
    forget_linear = mine[:, rows + lines : rows + 2 * lines].reshape(1, 1, length)
    head = lax.axis_index("tp")
    tap_weight = lax.dynamic_slice(conv_weight, (0, head * DK), (CONV, DK))
    keys = convolve(key_linear, tap_weight).reshape(1, 1, length, DK)
    weight_cache, first_read = read_cache(
        keys,
        values,
        input_linear,
        forget_linear,
        input_shift,
        forget_shift,
        new_query,
        new_key,
        new_value,
        new_input,
        new_forget,
    )
    return (keys, values, weight_cache, first_read)


def solution(mesh):
    in_specs = (
        P(("grp", "tp"), "sp", None),
        P(),
        P(),
        P(),
        P(),
        P(),
        P(),
        P(("grp", "sp"), "tp", None),
        P(("grp", "sp"), "tp", None),
        P(("grp", "sp"), "tp", None),
        P(("grp", "sp"), "tp", None),
        P(("grp", "sp"), "tp", None),
        P(("grp", "sp"), "tp"),
        P(("grp", "sp"), "tp"),
    )
    out_specs = (
        P(("grp", "sp"), "tp", None, None),
        P(("grp", "sp"), "tp", None, None),
        P(("grp", "sp"), "tp", None),
        P(("grp", "sp"), "tp", None),
    )
    return jax.shard_map(layer, mesh=mesh, in_specs=in_specs, out_specs=out_specs, check_vma=False)
```

```python
import jax
import jax.numpy as jnp
from jax import lax
from jax.sharding import PartitionSpec as P


HEADS = 8
DK = 128
CONV = 4


epsilon = 1e-06


def normalise(token_rows, norm_gain):
    widened = token_rows.astype(jnp.float32)
    return (
        widened
        * lax.rsqrt(jnp.mean(widened * widened, axis=-1, keepdims=True) + epsilon)
        * norm_gain.astype(jnp.float32)
    ).astype(jnp.bfloat16)


def project(normed, weight):
    matrix = weight.reshape(weight.shape[0], HEADS, DK)
    return jnp.einsum(
        "apd,dhk->hapk", normed, matrix, preferred_element_type=jnp.float32
    ).astype(jnp.bfloat16)


def gate(normed, weight):
    linear = jnp.einsum("apd,dh->hap", normed, weight, preferred_element_type=jnp.float32)
    return linear.astype(jnp.bfloat16)


def convolve(key_linear, tap_weight):
    length = key_linear.shape[0]
    extended = jnp.pad(key_linear.astype(jnp.float32), ((CONV - 1, 0), (0, 0)))
    summed = extended[0:length] * tap_weight[0]
    for offset in range(1, CONV):
        summed = summed + extended[offset : offset + length] * tap_weight[offset]
    return jax.nn.silu(summed).astype(jnp.bfloat16)


def read_cache(
    keys,
    values,
    input_linear,
    forget_linear,
    input_shift,
    forget_shift,
    new_query,
    new_key,
    new_value,
    new_input,
    new_forget,
):
    scaling = DK ** (-0.5)
    log_forget = jax.nn.log_sigmoid(forget_linear.astype(jnp.float32) + forget_shift)
    suffix = lax.cumsum(log_forget, axis=2, reverse=True) - log_forget
    new_decay = jax.nn.log_sigmoid(new_forget)
    base = lax.optimization_barrier(input_shift + new_decay[:, :, None])
    log_weight = input_linear.astype(jnp.float32) + base + suffix
    largest = jnp.maximum(jnp.max(log_weight, axis=2), new_input)
    weight_cache = jnp.exp(log_weight - largest[:, :, None])
    new_weight = jnp.exp(new_input - largest)
    fresh_match = jnp.sum(new_key.astype(jnp.float32) * new_query.astype(jnp.float32), axis=2)
    new_score = (new_weight * fresh_match * scaling).astype(jnp.bfloat16)
    matched = jnp.einsum("bhlk,bhk->bhl", keys, new_query, preferred_element_type=jnp.float32)
    scores = (weight_cache * matched * scaling).astype(jnp.bfloat16)
    denominator = jnp.sum(scores.astype(jnp.float32), axis=2)
    denominator = denominator + new_score.astype(jnp.float32)
    numerator = jnp.einsum("bhl,bhlk->bhk", scores, values, preferred_element_type=jnp.float32)
    numerator = numerator + new_score.astype(jnp.float32)[:, :, None] * new_value.astype(
        jnp.float32
    )
    first_read = (numerator / jnp.maximum(jnp.abs(denominator), 1.0)[:, :, None]).astype(
        jnp.bfloat16
    )
    return (weight_cache, first_read)


def trade(block):
    pair = block.shape[1]
    core = lax.axis_index("sp") % pair
    own = lax.dynamic_index_in_dim(block, core, 1, keepdims=False)
    other = lax.dynamic_index_in_dim(block, 1 - core, 1, keepdims=False)
    route = [(i, i ^ 1) for i in range(lax.axis_size("sp"))]
    got = lax.ppermute(other, "sp", route)
    first = core == 0
    return jnp.stack([jnp.where(first, own, got), jnp.where(first, got, own)], axis=1)


def rotate(block):
    ring = lax.axis_size("tp")
    here = lax.axis_index("tp")
    got = []
    for step in range(ring):
        mine = lax.dynamic_index_in_dim(block, (here + step) % ring, 0, keepdims=False)
        if step:
            route = [(i, (i + step) % ring) for i in range(ring)]
            mine = lax.ppermute(mine, "tp", route)
        got.append(mine)
    return jnp.stack(got)


def spread(stack):
    ring, chips = lax.axis_size("sp"), stack.shape[0]
    pair = ring // chips
    column, chip = lax.axis_index("tp"), lax.axis_index("sp") // pair
    whole = jnp.zeros_like(stack)
    for step in range(chips):
        target = (chip + step) % chips
        mine = lax.dynamic_index_in_dim(stack, (column - target) % chips, 0, keepdims=False)
        if step:
            route = [(i, (i // pair + step) % chips * pair + i % pair) for i in range(ring)]
            mine = lax.ppermute(mine, "sp", route)
        whole = lax.dynamic_update_index_in_dim(whole, mine, (chip - step) % chips, 0)
    return whole


def layer(
    layer_input,
    norm_gain,
    key_weight,
    value_weight,
    input_gate_weight,
    forget_gate_weight,
    conv_weight,
    input_shift,
    forget_shift,
    new_query,
    new_key,
    new_value,
    new_input,
    new_forget,
):
    seqs, rows, _ = layer_input.shape
    lines = rows // DK
    normed = normalise(layer_input, norm_gain)
    gates = jnp.stack(
        [gate(normed, input_gate_weight), gate(normed, forget_gate_weight)], axis=2
    ).reshape(HEADS, seqs, 2 * lines, DK)
    gates = jnp.pad(gates, ((0, 0), (0, 0), (0, 8 - 2 * lines), (0, 0)))
    key_block = jnp.concatenate([project(normed, key_weight), gates], axis=2)
    normed, key_block = lax.optimization_barrier((normed, key_block))
    value_block = project(normed, value_weight)
    value_block = trade(value_block).reshape(HEADS, seqs * rows, DK)
    mine = trade(spread(rotate(key_block)))
    mine = mine.reshape((-1,) + mine.shape[2:])
    values = spread(rotate(value_block))
    length = mine.shape[0] * rows
    key_linear = mine[:, :rows].reshape(length, DK)
    values = values.reshape(1, 1, length, DK)
    input_linear = mine[:, rows : rows + lines].reshape(1, 1, length)
    forget_linear = mine[:, rows + lines : rows + 2 * lines].reshape(1, 1, length)
    head = lax.axis_index("tp")
    tap_weight = lax.dynamic_slice(conv_weight, (0, head * DK), (CONV, DK))
    keys = convolve(key_linear, tap_weight).reshape(1, 1, length, DK)
    weight_cache, first_read = read_cache(
        keys,
        values,
        input_linear,
        forget_linear,
        input_shift,
        forget_shift,
        new_query,
        new_key,
        new_value,
        new_input,
        new_forget,
    )
    return (keys, values, weight_cache, first_read)


def solution(mesh):
    in_specs = (
        P(("grp", "tp"), "sp", None),
        P(),
        P(),
        P(),
        P(),
        P(),
        P(),
        P(("grp", "sp"), "tp", None),
        P(("grp", "sp"), "tp", None),
        P(("grp", "sp"), "tp", None),
        P(("grp", "sp"), "tp", None),
        P(("grp", "sp"), "tp", None),
        P(("grp", "sp"), "tp"),
        P(("grp", "sp"), "tp"),
    )
    out_specs = (
        P(("grp", "sp"), "tp", None, None),
        P(("grp", "sp"), "tp", None, None),
        P(("grp", "sp"), "tp", None),
        P(("grp", "sp"), "tp", None),
    )
    return jax.shard_map(layer, mesh=mesh, in_specs=in_specs, out_specs=out_specs, check_vma=False)
```

```python
import jax
import jax.numpy as jnp
from jax import lax
from jax.experimental import pallas as pl
from jax.experimental.pallas import tpu as pltpu
from jax.sharding import PartitionSpec as P


HEADS = 8
DK = 128
CONV = 4


epsilon = 1e-06


def project_kernel(place, x_hbm, gain, in_hbm, forget_hbm, key_hbm, value_hbm, *rest):
    *keys, kept, given, x, gate_weight, weight, normed, gates, x_sem, gate_sem, sem = rest
    step = pl.program_id(0)
    seqs, rows, lane = keys[0].shape[0], kept.shape[1], kept.shape[2]
    lines = rows // lane
    parts = x_sem.shape[0]
    part = x.shape[0] // parts
    chunk = 64

    def column(kind, shift):
        head = lax.rem(place[0] + shift, HEADS)
        source = (key_hbm, value_hbm)[kind].at[:, pl.ds(pl.multiple_of(head * lane, lane), lane)]
        half = shift % 2
        target = weight.at[kind, shift // 2, :, half * lane : (half + 1) * lane]
        return pltpu.make_async_copy(source, target, sem.at[kind, shift])

    def arrive(kind):
        for half in range(2):
            pltpu.make_async_copy(
                key_hbm.at[:, :lane],
                weight.at[kind, step, :, half * lane : (half + 1) * lane],
                sem.at[kind, 2 * step + half],
            ).wait()

    @pl.when(step == 0)
    def _():
        pieces = [
            pltpu.make_async_copy(
                x_hbm.at[n * part : (n + 1) * part], x.at[n * part : (n + 1) * part], x_sem.at[n]
            )
            for n in range(parts)
        ]
        gate_copies = [
            pltpu.make_async_copy(ref, gate_weight.at[n], gate_sem.at[n])
            for n, ref in enumerate((in_hbm, forget_hbm))
        ]
        for copy in pieces + gate_copies:
            copy.start()
        for shift in range(0, HEADS, 2):
            for kind in range(2):
                column(kind, shift).start()
                column(kind, shift + 1).start()
        scale = gain[...].astype(jnp.float32)
        for n in range(parts):
            pieces[n].wait()

            @pl.loop(0, part // chunk)
            def _(m):
                at = pl.ds(pl.multiple_of(n * part + m * chunk, chunk), chunk)
                wide = x[at, :].astype(jnp.float32)
                mean = jnp.mean(wide * wide, axis=-1, keepdims=True)
                normed[at, :] = (wide * lax.rsqrt(mean + epsilon) * scale).astype(jnp.bfloat16)

        for n in range(2):
            gate_copies[n].wait()
        both = jnp.concatenate([gate_weight[0], gate_weight[1]], axis=0)
        gates[...] = lax.dot_general(
            both, normed[...], (((1,), (1,)), ((), ())), preferred_element_type=jnp.float32
        )

    def dot(kind):
        arrive(kind)
        out = jnp.dot(normed[...], weight[kind, step], preferred_element_type=jnp.float32)
        return out.astype(jnp.bfloat16)

    key_rows = dot(0)
    tails = []
    for j in range(2):
        head = lax.rem(place[0] + 2 * step + j, HEADS)
        pair = [gates[pl.ds(head + HEADS * g, 1), :] for g in range(2)]
        for a in range(seqs):
            cut = [
                g[:, (a * lines + n) * lane : (a * lines + n + 1) * lane]
                for g in pair
                for n in range(lines)
            ]
            spare = jnp.zeros((8 - len(cut), lane), jnp.float32)
            tails.append(jnp.concatenate(cut + [spare], axis=0).astype(jnp.bfloat16))
    for c in range(HEADS // 2):

        @pl.when(step == c)
        def _():
            for j in range(2):
                for a in range(seqs):
                    block = key_rows[a * rows : (a + 1) * rows, j * lane : (j + 1) * lane]
                    keys[2 * c + j][a, :rows, :] = block
                    keys[2 * c + j][a, rows:, :] = tails[j * seqs + a]

    value_rows = dot(1)
    first = place[1] == 0
    for j in range(2):
        one = value_rows[:rows, j * lane : (j + 1) * lane]
        two = value_rows[rows:, j * lane : (j + 1) * lane]
        kept[j] = jnp.where(first, one, two)
        given[j] = jnp.where(first, two, one)


def project(place, layer_input, norm_gain, key_weight, value_weight, gate_in, gate_forget):
    seqs, rows, width = layer_input.shape
    tokens = seqs * rows

    def whole(*shape):
        return pl.BlockSpec(shape, lambda i, p: (0,) * len(shape))

    def halves():
        return pl.BlockSpec((2, rows, DK), lambda i, p: (i, 0, 0))

    hbm = pl.BlockSpec(memory_space=pltpu.MemorySpace.HBM)
    key_shape = (seqs, rows + 8, DK)
    value_shape = (HEADS, rows, DK)
    *keys, kept, given = pl.pallas_call(
        project_kernel,
        grid_spec=pltpu.PrefetchScalarGridSpec(
            num_scalar_prefetch=1,
            grid=(HEADS // 2,),
            in_specs=[hbm, whole(1, width), hbm, hbm, hbm, hbm],
            out_specs=[whole(*key_shape)] * HEADS + [halves(), halves()],
            scratch_shapes=[
                pltpu.VMEM((tokens, width), jnp.bfloat16),
                pltpu.VMEM((2, HEADS, width), jnp.bfloat16),
                pltpu.VMEM((2, HEADS // 2, width, 2 * DK), jnp.bfloat16),
                pltpu.VMEM((tokens, width), jnp.bfloat16),
                pltpu.VMEM((2 * HEADS, tokens), jnp.float32),
                pltpu.SemaphoreType.DMA((4,)),
                pltpu.SemaphoreType.DMA((2,)),
                pltpu.SemaphoreType.DMA((2, HEADS)),
            ],
        ),
        out_shape=[jax.ShapeDtypeStruct(key_shape, jnp.bfloat16)] * HEADS
        + [jax.ShapeDtypeStruct(value_shape, jnp.bfloat16)] * 2,
        compiler_params=pltpu.CompilerParams(
            dimension_semantics=("arbitrary",), vmem_limit_bytes=60 * 1024 * 1024
        ),
        cost_estimate=pl.CostEstimate(
            flops=4 * tokens * width * HEADS * DK,
            bytes_accessed=2 * (tokens * width + 2 * width * HEADS * DK + 2 * tokens * HEADS * DK),
            transcendentals=tokens,
        ),
        name="project",
    )(
        place,
        layer_input.reshape(tokens, width),
        norm_gain.reshape(1, width),
        gate_in.T,
        gate_forget.T,
        key_weight,
        value_weight,
    )
    return keys, kept, given


def convolve(key_linear, tap_weight):
    length = key_linear.shape[0]
    extended = jnp.pad(key_linear.astype(jnp.float32), ((CONV - 1, 0), (0, 0)))
    summed = extended[0:length] * tap_weight[0]
    for offset in range(1, CONV):
        summed = summed + extended[offset : offset + length] * tap_weight[offset]
    return jax.nn.silu(summed).astype(jnp.bfloat16)


def read_cache(
    keys,
    values,
    input_linear,
    forget_linear,
    input_shift,
    forget_shift,
    new_query,
    new_key,
    new_value,
    new_input,
    new_forget,
):
    scaling = DK ** (-0.5)
    log_forget = jax.nn.log_sigmoid(forget_linear.astype(jnp.float32) + forget_shift)
    suffix = lax.cumsum(log_forget, axis=2, reverse=True) - log_forget
    new_decay = jax.nn.log_sigmoid(new_forget)
    base = lax.optimization_barrier(input_shift + new_decay[:, :, None])
    log_weight = input_linear.astype(jnp.float32) + base + suffix
    largest = jnp.maximum(jnp.max(log_weight, axis=2), new_input)
    weight_cache = jnp.exp(log_weight - largest[:, :, None])
    new_weight = jnp.exp(new_input - largest)
    fresh_match = jnp.sum(new_key.astype(jnp.float32) * new_query.astype(jnp.float32), axis=2)
    new_score = (new_weight * fresh_match * scaling).astype(jnp.bfloat16)
    matched = jnp.einsum("bhlk,bhk->bhl", keys, new_query, preferred_element_type=jnp.float32)
    scores = (weight_cache * matched * scaling).astype(jnp.bfloat16)
    denominator = jnp.sum(scores.astype(jnp.float32), axis=2)
    denominator = denominator + new_score.astype(jnp.float32)
    numerator = jnp.einsum("bhl,bhlk->bhk", scores, values, preferred_element_type=jnp.float32)
    numerator = numerator + new_score.astype(jnp.float32)[:, :, None] * new_value.astype(
        jnp.float32
    )
    first_read = (numerator / jnp.maximum(jnp.abs(denominator), 1.0)[:, :, None]).astype(
        jnp.bfloat16
    )
    return (weight_cache, first_read)


def trade(own, other):
    first = lax.axis_index("sp") % 2 == 0
    route = [(i, i ^ 1) for i in range(lax.axis_size("sp"))]
    got = lax.ppermute(other, "sp", route)
    return jnp.stack([jnp.where(first, own, got), jnp.where(first, got, own)], axis=1)


def rotate(blocks):
    ring = lax.axis_size("tp")
    got = list(blocks[:1])
    for step in range(1, ring):
        route = [(i, (i + step) % ring) for i in range(ring)]
        got.append(lax.ppermute(blocks[step], "tp", route))
    return jnp.stack(got)


def spread(stack):
    ring, chips = lax.axis_size("sp"), stack.shape[0]
    pair = ring // chips
    column, chip = lax.axis_index("tp"), lax.axis_index("sp") // pair
    whole = jnp.zeros_like(stack)
    for step in range(chips):
        target = (chip + step) % chips
        mine = lax.dynamic_index_in_dim(stack, (column - target) % chips, 0, keepdims=False)
        if step:
            route = [(i, (i // pair + step) % chips * pair + i % pair) for i in range(ring)]
            mine = lax.ppermute(mine, "sp", route)
        whole = lax.dynamic_update_index_in_dim(whole, mine, (chip - step) % chips, 0)
    return whole


def layer(
    layer_input,
    norm_gain,
    key_weight,
    value_weight,
    input_gate_weight,
    forget_gate_weight,
    conv_weight,
    input_shift,
    forget_shift,
    new_query,
    new_key,
    new_value,
    new_input,
    new_forget,
):
    seqs, rows, _ = layer_input.shape
    lines = rows // DK
    core = lax.axis_index("sp") % 2
    place = jnp.stack([lax.axis_index("tp"), core]).astype(jnp.int32)
    key_blocks, kept, given = project(
        place,
        layer_input,
        norm_gain,
        key_weight,
        value_weight,
        input_gate_weight,
        forget_gate_weight,
    )
    value_blocks = trade(kept, given).reshape(HEADS, seqs * rows, DK)
    mine = spread(rotate(key_blocks))
    own = lax.dynamic_index_in_dim(mine, core, 1, keepdims=False)
    other = lax.dynamic_index_in_dim(mine, 1 - core, 1, keepdims=False)
    mine = trade(own, other).reshape((-1,) + own.shape[1:])
    values = spread(rotate(value_blocks))
    length = mine.shape[0] * rows
    key_linear = mine[:, :rows].reshape(length, DK)
    values = values.reshape(1, 1, length, DK)
    input_linear = mine[:, rows : rows + lines].reshape(1, 1, length)
    forget_linear = mine[:, rows + lines : rows + 2 * lines].reshape(1, 1, length)
    head = lax.axis_index("tp")
    tap_weight = lax.dynamic_slice(conv_weight, (0, head * DK), (CONV, DK))
    keys = convolve(key_linear, tap_weight).reshape(1, 1, length, DK)
    weight_cache, first_read = read_cache(
        keys,
        values,
        input_linear,
        forget_linear,
        input_shift,
        forget_shift,
        new_query,
        new_key,
        new_value,
        new_input,
        new_forget,
    )
    return (keys, values, weight_cache, first_read)


def solution(mesh):
    in_specs = (
        P(("grp", "tp"), "sp", None),
        P(),
        P(),
        P(),
        P(),
        P(),
        P(),
        P(("grp", "sp"), "tp", None),
        P(("grp", "sp"), "tp", None),
        P(("grp", "sp"), "tp", None),
        P(("grp", "sp"), "tp", None),
        P(("grp", "sp"), "tp", None),
        P(("grp", "sp"), "tp"),
        P(("grp", "sp"), "tp"),
    )
    out_specs = (
        P(("grp", "sp"), "tp", None, None),
        P(("grp", "sp"), "tp", None, None),
        P(("grp", "sp"), "tp", None),
        P(("grp", "sp"), "tp", None),
    )
    return jax.shard_map(layer, mesh=mesh, in_specs=in_specs, out_specs=out_specs, check_vma=False)
```

```python
import jax
import jax.numpy as jnp
from jax import lax
from jax.experimental import pallas as pl
from jax.experimental.pallas import tpu as pltpu
from jax.sharding import PartitionSpec as P


HEADS = 8
DK = 128
CONV = 4


epsilon = 1e-06


def project_kernel(x_hbm, gain, in_hbm, forget_hbm, key_hbm, value_hbm, *rest):
    *keys, kept, given, x, gate_weight, weight, normed, gates, x_sem, gate_sem, sem = rest
    step = pl.program_id(0)
    seqs, rows, lane = keys[0].shape[0], kept.shape[1], kept.shape[2]
    lines = rows // lane
    parts = x_sem.shape[0]
    part = x.shape[0] // parts
    chunk = 16
    pieces = [
        pltpu.make_async_copy(
            x_hbm.at[n * part : (n + 1) * part], x.at[n * part : (n + 1) * part], x_sem.at[n]
        )
        for n in range(parts)
    ]
    gate_copies = [
        pltpu.make_async_copy(ref, gate_weight.at[n], gate_sem.at[n])
        for n, ref in enumerate((in_hbm, forget_hbm))
    ]
    weight_copies = [
        pltpu.make_async_copy(ref, weight.at[n], sem.at[n])
        for n, ref in enumerate((key_hbm, value_hbm))
    ]

    @pl.when(step == 0)
    def _():
        for copy in pieces + gate_copies + weight_copies:
            copy.start()
        fine = gain[...].astype(jnp.float32)
        scale = jnp.concatenate([fine[n : n + 1] for n in range(fine.shape[0])], axis=1)
        for n in range(parts):
            pieces[n].wait()

            @pl.loop(0, part // chunk)
            def _(m):
                at = pl.ds(pl.multiple_of(n * part + m * chunk, chunk), chunk)
                wide = x[at, :].astype(jnp.float32)
                mean = jnp.mean(wide * wide, axis=-1, keepdims=True)
                normed[at, :] = (wide * lax.rsqrt(mean + epsilon) * scale).astype(jnp.bfloat16)

        for n in range(2):
            gate_copies[n].wait()
        both = jnp.concatenate([gate_weight[0], gate_weight[1]], axis=0)
        across = lax.dot_general(
            normed[...], both, (((1,), (1,)), ((), ())), preferred_element_type=jnp.float32
        )
        gates[...] = across.T
        weight_copies[0].wait()

    heads = [lax.rem(lax.axis_index("tp") + 2 * step + j, HEADS) for j in range(2)]

    def dot(kind):
        sides = [weight[kind, :, pl.ds(pl.multiple_of(h * lane, lane), lane)] for h in heads]
        out = jnp.dot(
            normed[...], jnp.concatenate(sides, axis=1), preferred_element_type=jnp.float32
        )
        return out.astype(jnp.bfloat16)

    key_rows = dot(0)
    tails = []
    for head in heads:
        pair = [gates[pl.ds(head + HEADS * g, 1), :] for g in range(2)]
        for a in range(seqs):
            cut = [
                g[:, (a * lines + n) * lane : (a * lines + n + 1) * lane]
                for g in pair
                for n in range(lines)
            ]
            spare = jnp.zeros((8 - len(cut), lane), jnp.float32)
            tails.append(jnp.concatenate(cut + [spare], axis=0).astype(jnp.bfloat16))
    for c in range(HEADS // 2):

        @pl.when(step == c)
        def _():
            for j in range(2):
                for a in range(seqs):
                    block = key_rows[a * rows : (a + 1) * rows, j * lane : (j + 1) * lane]
                    keys[2 * c + j][a, :rows, :] = block
                    keys[2 * c + j][a, rows:, :] = tails[j * seqs + a]

    @pl.when(step == 0)
    def _():
        weight_copies[1].wait()

    value_rows = dot(1)
    first = lax.rem(lax.axis_index("sp"), 2) == 0
    for j in range(2):
        one = value_rows[:rows, j * lane : (j + 1) * lane]
        two = value_rows[rows:, j * lane : (j + 1) * lane]
        kept[j] = jnp.where(first, one, two)
        given[j] = jnp.where(first, two, one)


def project(layer_input, norm_gain, key_weight, value_weight, gate_in, gate_forget):
    seqs, rows, width = layer_input.shape
    tokens = seqs * rows

    def whole(*shape):
        return pl.BlockSpec(shape, lambda i: (0,) * len(shape))

    def halves():
        return pl.BlockSpec((2, rows, DK), lambda i: (i, 0, 0))

    hbm = pl.BlockSpec(memory_space=pl.ANY)
    key_shape = (seqs, rows + 8, DK)
    value_shape = (HEADS, rows, DK)
    *keys, kept, given = pl.pallas_call(
        project_kernel,
        grid=(HEADS // 2,),
        in_specs=[hbm, whole(width // DK, DK), hbm, hbm, hbm, hbm],
        out_specs=[whole(*key_shape)] * HEADS + [halves(), halves()],
        scratch_shapes=[
            pltpu.VMEM((tokens, width), jnp.bfloat16),
            pltpu.VMEM((2, HEADS, width), jnp.bfloat16),
            pltpu.VMEM((2, width, HEADS * DK), jnp.bfloat16),
            pltpu.VMEM((tokens, width), jnp.bfloat16),
            pltpu.VMEM((2 * HEADS, tokens), jnp.float32),
            pltpu.SemaphoreType.DMA((4,)),
            pltpu.SemaphoreType.DMA((2,)),
            pltpu.SemaphoreType.DMA((2,)),
        ],
        out_shape=[jax.ShapeDtypeStruct(key_shape, jnp.bfloat16)] * HEADS
        + [jax.ShapeDtypeStruct(value_shape, jnp.bfloat16)] * 2,
        compiler_params=pltpu.CompilerParams(
            dimension_semantics=("arbitrary",), vmem_limit_bytes=60 * 1024 * 1024
        ),
        cost_estimate=pl.CostEstimate(
            flops=4 * tokens * width * HEADS * DK,
            bytes_accessed=2 * (tokens * width + 2 * width * HEADS * DK + 2 * tokens * HEADS * DK),
            transcendentals=tokens,
        ),
        name="project",
    )(
        layer_input.reshape(tokens, width),
        norm_gain.reshape(width // DK, DK),
        gate_in.T,
        gate_forget.T,
        key_weight,
        value_weight,
    )
    return keys, kept, given


def finish_kernel(scores, fresh, bottom, new_value, *rest):
    chips = scores.shape[0]
    *blocks, cache, read, held, in_sem, out_sem = rest
    chip = lax.axis_index("sp") // 2
    moves = [pltpu.make_async_copy(b, held.at[n], in_sem.at[n]) for n, b in enumerate(blocks)]
    for move in moves:
        move.start()
    total = fresh[0, 0] * new_value[...].astype(jnp.float32)
    stores = []
    for n in range(chips):
        source = lax.rem(chip - n + chips, chips)
        moves[n].wait()
        stores.append(pltpu.make_async_copy(held.at[n], cache.at[source], out_sem.at[n]))
        stores[n].start()
        block = held[n]
        row = jnp.broadcast_to(scores[pl.ds(source, 1), :], (8, scores.shape[1]))
        part = jnp.dot(
            row.astype(jnp.bfloat16),
            block.reshape(-1, block.shape[-1]),
            preferred_element_type=jnp.float32,
        )
        total = total + part[:1]
    read[...] = (total / jnp.maximum(jnp.abs(bottom[0, 0]), 1.0)).astype(jnp.bfloat16)
    for store in stores:
        store.wait()


def finish(blocks, scores, new_score, denominator, new_value):
    chips, shape = len(blocks), blocks[0].shape
    vmem, smem = (pl.BlockSpec(memory_space=m) for m in (pltpu.VMEM, pltpu.SMEM))
    anywhere = pl.BlockSpec(memory_space=pl.ANY)
    cache, read = pl.pallas_call(
        finish_kernel,
        in_specs=[vmem, smem, smem, vmem] + [anywhere] * chips,
        out_specs=[anywhere, vmem],
        scratch_shapes=[
            pltpu.VMEM((chips,) + shape, jnp.bfloat16),
            pltpu.SemaphoreType.DMA((chips,)),
            pltpu.SemaphoreType.DMA((chips,)),
        ],
        out_shape=[
            jax.ShapeDtypeStruct((chips,) + shape, jnp.bfloat16),
            jax.ShapeDtypeStruct((1, DK), jnp.bfloat16),
        ],
        compiler_params=pltpu.CompilerParams(vmem_limit_bytes=60 * 1024 * 1024),
        name="finish",
    )(
        scores.astype(jnp.float32).reshape(chips, -1),
        new_score.astype(jnp.float32),
        denominator,
        new_value.reshape(1, DK),
        *blocks,
    )
    return cache, read


def convolve(key_linear, tap_weight):
    length = key_linear.shape[0]
    extended = jnp.pad(key_linear.astype(jnp.float32), ((CONV - 1, 0), (0, 0)))
    summed = extended[0:length] * tap_weight[0]
    for offset in range(1, CONV):
        summed = summed + extended[offset : offset + length] * tap_weight[offset]
    return jax.nn.silu(summed).astype(jnp.bfloat16)


def read_cache(
    keys,
    values,
    input_linear,
    forget_linear,
    input_shift,
    forget_shift,
    new_query,
    new_key,
    new_value,
    new_input,
    new_forget,
):
    scaling = DK ** (-0.5)
    log_forget = jax.nn.log_sigmoid(forget_linear.astype(jnp.float32) + forget_shift)
    suffix = lax.cumsum(log_forget, axis=2, reverse=True) - log_forget
    new_decay = jax.nn.log_sigmoid(new_forget)
    base = lax.optimization_barrier(input_shift + new_decay[:, :, None])
    log_weight = input_linear.astype(jnp.float32) + base + suffix
    largest = jnp.maximum(jnp.max(log_weight, axis=2), new_input)
    weight_cache = jnp.exp(log_weight - largest[:, :, None])
    new_weight = jnp.exp(new_input - largest)
    fresh_match = jnp.sum(new_key.astype(jnp.float32) * new_query.astype(jnp.float32), axis=2)
    new_score = (new_weight * fresh_match * scaling).astype(jnp.bfloat16)
    matched = jnp.einsum("bhlk,bhk->bhl", keys, new_query, preferred_element_type=jnp.float32)
    scores = (weight_cache * matched * scaling).astype(jnp.bfloat16)
    denominator = jnp.sum(scores.astype(jnp.float32), axis=2)
    denominator = denominator + new_score.astype(jnp.float32)
    cache, first_read = finish(values, scores, new_score, denominator, new_value)
    return (cache, weight_cache, first_read)


def trade(own, other):
    first = lax.axis_index("sp") % 2 == 0
    route = [(i, i ^ 1) for i in range(lax.axis_size("sp"))]
    got = lax.ppermute(other, "sp", route)
    return jnp.stack([jnp.where(first, own, got), jnp.where(first, got, own)], axis=1)


def rotate(blocks):
    ring = lax.axis_size("tp")
    got = list(blocks[:1])
    for step in range(1, ring):
        route = [(i, (i + step) % ring) for i in range(ring)]
        got.append(lax.ppermute(blocks[step], "tp", route))
    return jnp.stack(got)


def spread(stack):
    ring, chips = lax.axis_size("sp"), stack.shape[0]
    pair = ring // chips
    column, chip = lax.axis_index("tp"), lax.axis_index("sp") // pair
    got = []
    for step in range(chips):
        target = (chip + step) % chips
        mine = lax.dynamic_index_in_dim(stack, (column - target) % chips, 0, keepdims=False)
        if step:
            route = [(i, (i // pair + step) % chips * pair + i % pair) for i in range(ring)]
            mine = lax.ppermute(mine, "sp", route)
        got.append(mine)
    return got


def in_order(blocks):
    chips = len(blocks)
    chip = lax.axis_index("sp") * chips // lax.axis_size("sp")
    whole = jnp.zeros((chips,) + blocks[0].shape, blocks[0].dtype)
    for step, block in enumerate(blocks):
        whole = lax.dynamic_update_index_in_dim(whole, block, (chip - step) % chips, 0)
    return whole


def layer(
    layer_input,
    norm_gain,
    key_weight,
    value_weight,
    input_gate_weight,
    forget_gate_weight,
    conv_weight,
    input_shift,
    forget_shift,
    new_query,
    new_key,
    new_value,
    new_input,
    new_forget,
):
    _, rows, _ = layer_input.shape
    lines = rows // DK
    core = lax.axis_index("sp") % 2
    key_blocks, kept, given = project(
        layer_input,
        norm_gain,
        key_weight,
        value_weight,
        input_gate_weight,
        forget_gate_weight,
    )
    value_blocks = trade(kept, given)
    mine = in_order(spread(rotate(key_blocks)))
    own = lax.dynamic_index_in_dim(mine, core, 1, keepdims=False)
    other = lax.dynamic_index_in_dim(mine, 1 - core, 1, keepdims=False)
    mine = trade(own, other).reshape((-1,) + own.shape[1:])
    values = spread(rotate(value_blocks))
    length = mine.shape[0] * rows
    key_linear = mine[:, :rows].reshape(length, DK)
    input_linear = mine[:, rows : rows + lines].reshape(1, 1, length)
    forget_linear = mine[:, rows + lines : rows + 2 * lines].reshape(1, 1, length)
    head = lax.axis_index("tp")
    tap_weight = lax.dynamic_slice(conv_weight, (0, head * DK), (CONV, DK))
    keys = convolve(key_linear, tap_weight).reshape(1, 1, length, DK)
    values, weight_cache, first_read = read_cache(
        keys,
        values,
        input_linear,
        forget_linear,
        input_shift,
        forget_shift,
        new_query,
        new_key,
        new_value,
        new_input,
        new_forget,
    )
    return (keys, values.reshape(keys.shape), weight_cache, first_read.reshape(new_value.shape))


def solution(mesh):
    in_specs = (
        P(("grp", "tp"), "sp", None),
        P(),
        P(),
        P(),
        P(),
        P(),
        P(),
        P(("grp", "sp"), "tp", None),
        P(("grp", "sp"), "tp", None),
        P(("grp", "sp"), "tp", None),
        P(("grp", "sp"), "tp", None),
        P(("grp", "sp"), "tp", None),
        P(("grp", "sp"), "tp"),
        P(("grp", "sp"), "tp"),
    )
    out_specs = (
        P(("grp", "sp"), "tp", None, None),
        P(("grp", "sp"), "tp", None, None),
        P(("grp", "sp"), "tp", None),
        P(("grp", "sp"), "tp", None),
    )
    return jax.shard_map(layer, mesh=mesh, in_specs=in_specs, out_specs=out_specs, check_vma=False)
```

```python
import jax
import jax.numpy as jnp
from jax import lax
from jax.experimental import pallas as pl
from jax.experimental.pallas import tpu as pltpu
from jax.sharding import PartitionSpec as P


HEADS = 8
DK = 128
CONV = 4


epsilon = 1e-06


EXTRA = 8
TUNING = dict(dimension_semantics=("arbitrary",))


def two_heads(step, lane):
    heads = [lax.rem(lax.axis_index("tp") + 2 * step + j, HEADS) for j in range(2)]
    return heads, [pl.ds(pl.multiple_of(h * lane, lane), lane) for h in heads]


def key_kernel(x_hbm, gain, in_hbm, forget_hbm, key_hbm, *rest):
    *keys, normed_hbm, x, gate_weight, weight, normed, gates, x_sem, gate_sem, sem, out_sem = rest
    step = pl.program_id(0)
    steps = HEADS // 2
    seqs, lane = keys[0].shape[0], keys[0].shape[2]
    rows = keys[0].shape[1] - EXTRA
    lines = rows // lane
    parts = x_sem.shape[0]
    part = x.shape[0] // parts
    chunk = 16
    keep = pltpu.make_async_copy(normed, normed_hbm, out_sem)

    def fetch(at):
        _, columns = two_heads(at, lane)
        return [
            pltpu.make_async_copy(
                key_hbm.at[:, c], weight.at[at, :, j * lane : (j + 1) * lane], sem.at[at, j]
            )
            for j, c in enumerate(columns)
        ]

    @pl.when(step == 0)
    def _():
        pieces = [
            pltpu.make_async_copy(
                x_hbm.at[n * part : (n + 1) * part], x.at[n * part : (n + 1) * part], x_sem.at[n]
            )
            for n in range(parts)
        ]
        gate_copies = [
            pltpu.make_async_copy(ref, gate_weight.at[n], gate_sem.at[n])
            for n, ref in enumerate((in_hbm, forget_hbm))
        ]
        for copy in pieces + gate_copies:
            copy.start()
        for n in range(steps):
            for copy in fetch(n):
                copy.start()
        fine = gain[...].astype(jnp.float32)
        scale = jnp.concatenate([fine[n : n + 1] for n in range(fine.shape[0])], axis=1)
        for n in range(parts):
            pieces[n].wait()

            @pl.loop(0, part // chunk)
            def _(m):
                at = pl.ds(pl.multiple_of(n * part + m * chunk, chunk), chunk)
                wide = x[at, :].astype(jnp.float32)
                mean = jnp.mean(wide * wide, axis=-1, keepdims=True)
                normed[at, :] = (wide * lax.rsqrt(mean + epsilon) * scale).astype(jnp.bfloat16)

        keep.start()
        for n in range(2):
            gate_copies[n].wait()
        both = jnp.concatenate([gate_weight[0], gate_weight[1]], axis=0)
        across = lax.dot_general(
            normed[...], both, (((1,), (1,)), ((), ())), preferred_element_type=jnp.float32
        )
        gates[...] = across.T

    for copy in fetch(step):
        copy.wait()
    key_rows = jnp.dot(normed[...], weight[step], preferred_element_type=jnp.float32)
    key_rows = key_rows.astype(jnp.bfloat16)
    heads, _ = two_heads(step, lane)
    tails = []
    for head in heads:
        pair = [gates[pl.ds(head + HEADS * g, 1), :] for g in range(2)]
        for a in range(seqs):
            cut = [
                g[:, (a * lines + n) * lane : (a * lines + n + 1) * lane]
                for g in pair
                for n in range(lines)
            ]
            spare = jnp.zeros((EXTRA - len(cut), lane), jnp.float32)
            tails.append(jnp.concatenate(cut + [spare], axis=0).astype(jnp.bfloat16))
    for c in range(steps):

        @pl.when(step == c)
        def _():
            for j in range(2):
                for a in range(seqs):
                    block = key_rows[a * rows : (a + 1) * rows, j * lane : (j + 1) * lane]
                    keys[2 * c + j][a, :rows, :] = block
                    keys[2 * c + j][a, rows:, :] = tails[j * seqs + a]

    @pl.when(step == steps - 1)
    def _():
        keep.wait()


def project_keys(layer_input, norm_gain, key_weight, gate_in, gate_forget):
    seqs, rows, width = layer_input.shape
    tokens = seqs * rows

    def whole(*shape):
        return pl.BlockSpec(shape, lambda i: (0,) * len(shape))

    anywhere = pl.BlockSpec(memory_space=pl.ANY)
    key_shape = (seqs, rows + EXTRA, DK)
    *keys, normed = pl.pallas_call(
        key_kernel,
        grid=(HEADS // 2,),
        in_specs=[anywhere, whole(width // DK, DK), anywhere, anywhere, anywhere],
        out_specs=[whole(*key_shape)] * HEADS + [anywhere],
        scratch_shapes=[
            pltpu.VMEM((tokens, width), jnp.bfloat16),
            pltpu.VMEM((2, HEADS, width), jnp.bfloat16),
            pltpu.VMEM((HEADS // 2, width, 2 * DK), jnp.bfloat16),
            pltpu.VMEM((tokens, width), jnp.bfloat16),
            pltpu.VMEM((2 * HEADS, tokens), jnp.float32),
            pltpu.SemaphoreType.DMA((4,)),
            pltpu.SemaphoreType.DMA((2,)),
            pltpu.SemaphoreType.DMA((HEADS // 2, 2)),
            pltpu.SemaphoreType.DMA,
        ],
        out_shape=[jax.ShapeDtypeStruct(key_shape, jnp.bfloat16)] * HEADS
        + [jax.ShapeDtypeStruct((tokens, width), jnp.bfloat16)],
        compiler_params=pltpu.CompilerParams(vmem_limit_bytes=60 * 1024 * 1024, **TUNING),
        cost_estimate=pl.CostEstimate(
            flops=2 * tokens * width * HEADS * DK,
            bytes_accessed=2 * (tokens * width + width * HEADS * DK + tokens * HEADS * DK),
            transcendentals=tokens,
        ),
        name="project_keys",
    )(
        layer_input.reshape(tokens, width),
        norm_gain.reshape(width // DK, DK),
        gate_in.T,
        gate_forget.T,
        key_weight,
    )
    return keys, normed


def value_kernel(normed_any, weight_any, kept, given, normed, weight, sem):
    step = pl.program_id(0)
    lane = kept.shape[2]
    rows = kept.shape[1] - EXTRA

    @pl.when(step == 0)
    def _():
        copies = [
            pltpu.make_async_copy(normed_any, normed, sem.at[0]),
            pltpu.make_async_copy(weight_any, weight, sem.at[1]),
        ]
        for copy in copies:
            copy.start()
        for copy in copies:
            copy.wait()

    _, columns = two_heads(step, lane)
    sides = jnp.concatenate([weight[:, c] for c in columns], axis=1)
    value_rows = jnp.dot(normed[...], sides, preferred_element_type=jnp.float32)
    value_rows = value_rows.astype(jnp.bfloat16)
    first = lax.rem(lax.axis_index("sp"), 2) == 0
    for j in range(2):
        one = value_rows[:rows, j * lane : (j + 1) * lane]
        two = value_rows[rows:, j * lane : (j + 1) * lane]
        kept[j, :rows, :] = jnp.where(first, one, two)
        given[j, :rows, :] = jnp.where(first, two, one)
        kept[j, rows:, :] = jnp.zeros((EXTRA, lane), kept.dtype)
        given[j, rows:, :] = jnp.zeros((EXTRA, lane), given.dtype)


def project_values(normed, value_weight, rows):
    tokens, width = normed.shape
    anywhere = pl.BlockSpec(memory_space=pl.ANY)
    half = pl.BlockSpec((2, rows + EXTRA, DK), lambda i: (i, 0, 0))
    return pl.pallas_call(
        value_kernel,
        grid=(HEADS // 2,),
        in_specs=[anywhere, anywhere],
        out_specs=[half, half],
        scratch_shapes=[
            pltpu.VMEM(normed.shape, jnp.bfloat16),
            pltpu.VMEM(value_weight.shape, jnp.bfloat16),
            pltpu.SemaphoreType.DMA((2,)),
        ],
        out_shape=[jax.ShapeDtypeStruct((HEADS, rows + EXTRA, DK), jnp.bfloat16)] * 2,
        compiler_params=pltpu.CompilerParams(vmem_limit_bytes=20 * 1024 * 1024, **TUNING),
        cost_estimate=pl.CostEstimate(
            flops=2 * tokens * width * HEADS * DK,
            bytes_accessed=2 * (tokens * width + width * HEADS * DK + tokens * HEADS * DK),
            transcendentals=0,
        ),
        name="project_values",
    )(normed, value_weight)


def finish_kernel(scores, fresh, bottom, new_value, *rest):
    chips = scores.shape[0]
    *blocks, cache, read, held, in_sem, out_sem = rest
    rows = cache.shape[2]
    chip = lax.axis_index("sp") // 2
    moves = [pltpu.make_async_copy(b, held.at[n], in_sem.at[n]) for n, b in enumerate(blocks)]
    for move in moves:
        move.start()
    total = fresh[0, 0] * new_value[...].astype(jnp.float32)
    stores = []
    for n in range(chips):
        source = lax.rem(chip - n + chips, chips)
        moves[n].wait()
        stores.append(pltpu.make_async_copy(held.at[n, :, :rows], cache.at[source], out_sem.at[n]))
        stores[n].start()
        block = held[n, :, :rows]
        row = jnp.broadcast_to(scores[pl.ds(source, 1), :], (8, scores.shape[1]))
        part = jnp.dot(
            row.astype(jnp.bfloat16),
            block.reshape(-1, block.shape[-1]),
            preferred_element_type=jnp.float32,
        )
        total = total + part[:1]
    read[...] = (total / jnp.maximum(jnp.abs(bottom[0, 0]), 1.0)).astype(jnp.bfloat16)
    for store in stores:
        store.wait()


def finish(blocks, scores, new_score, denominator, new_value):
    chips, shape = len(blocks), blocks[0].shape
    vmem, smem = (pl.BlockSpec(memory_space=m) for m in (pltpu.VMEM, pltpu.SMEM))
    anywhere = pl.BlockSpec(memory_space=pl.ANY)
    cache, read = pl.pallas_call(
        finish_kernel,
        in_specs=[vmem, smem, smem, vmem] + [anywhere] * chips,
        out_specs=[anywhere, vmem],
        scratch_shapes=[
            pltpu.VMEM((chips,) + shape, jnp.bfloat16),
            pltpu.SemaphoreType.DMA((chips,)),
            pltpu.SemaphoreType.DMA((chips,)),
        ],
        out_shape=[
            jax.ShapeDtypeStruct((chips, shape[0], shape[1] - EXTRA, DK), jnp.bfloat16),
            jax.ShapeDtypeStruct((1, DK), jnp.bfloat16),
        ],
        compiler_params=pltpu.CompilerParams(vmem_limit_bytes=60 * 1024 * 1024),
        name="finish",
    )(
        scores.astype(jnp.float32).reshape(chips, -1),
        new_score.astype(jnp.float32),
        denominator,
        new_value.reshape(1, DK),
        *blocks,
    )
    return cache, read


def convolve(key_linear, tap_weight):
    length = key_linear.shape[0]
    extended = jnp.pad(key_linear.astype(jnp.float32), ((CONV - 1, 0), (0, 0)))
    summed = extended[0:length] * tap_weight[0]
    for offset in range(1, CONV):
        summed = summed + extended[offset : offset + length] * tap_weight[offset]
    return jax.nn.silu(summed).astype(jnp.bfloat16)


def read_cache(
    keys,
    values,
    input_linear,
    forget_linear,
    input_shift,
    forget_shift,
    new_query,
    new_key,
    new_value,
    new_input,
    new_forget,
):
    scaling = DK ** (-0.5)
    log_forget = jax.nn.log_sigmoid(forget_linear.astype(jnp.float32) + forget_shift)
    suffix = lax.cumsum(log_forget, axis=2, reverse=True) - log_forget
    new_decay = jax.nn.log_sigmoid(new_forget)
    base = lax.optimization_barrier(input_shift + new_decay[:, :, None])
    log_weight = input_linear.astype(jnp.float32) + base + suffix
    largest = jnp.maximum(jnp.max(log_weight, axis=2), new_input)
    weight_cache = jnp.exp(log_weight - largest[:, :, None])
    new_weight = jnp.exp(new_input - largest)
    fresh_match = jnp.sum(new_key.astype(jnp.float32) * new_query.astype(jnp.float32), axis=2)
    new_score = (new_weight * fresh_match * scaling).astype(jnp.bfloat16)
    matched = jnp.einsum("bhlk,bhk->bhl", keys, new_query, preferred_element_type=jnp.float32)
    scores = (weight_cache * matched * scaling).astype(jnp.bfloat16)
    denominator = jnp.sum(scores.astype(jnp.float32), axis=2)
    denominator = denominator + new_score.astype(jnp.float32)
    cache, first_read = finish(values, scores, new_score, denominator, new_value)
    return (cache, weight_cache, first_read)


def trade(own, other):
    first = lax.axis_index("sp") % 2 == 0
    route = [(i, i ^ 1) for i in range(lax.axis_size("sp"))]
    got = lax.ppermute(other, "sp", route)
    return jnp.stack([jnp.where(first, own, got), jnp.where(first, got, own)], axis=1)


def rotate(blocks):
    ring = lax.axis_size("tp")
    got = list(blocks[:1])
    for step in range(1, ring):
        route = [(i, (i + step) % ring) for i in range(ring)]
        got.append(lax.ppermute(blocks[step], "tp", route))
    return jnp.stack(got)


def spread(stack):
    ring, chips = lax.axis_size("sp"), stack.shape[0]
    pair = ring // chips
    column, chip = lax.axis_index("tp"), lax.axis_index("sp") // pair
    got = []
    for step in range(chips):
        target = (chip + step) % chips
        mine = lax.dynamic_index_in_dim(stack, (column - target) % chips, 0, keepdims=False)
        if step:
            route = [(i, (i // pair + step) % chips * pair + i % pair) for i in range(ring)]
            mine = lax.ppermute(mine, "sp", route)
        got.append(mine)
    return got


def in_order(blocks):
    chips = len(blocks)
    chip = lax.axis_index("sp") * chips // lax.axis_size("sp")
    whole = jnp.zeros((chips,) + blocks[0].shape, blocks[0].dtype)
    for step, block in enumerate(blocks):
        whole = lax.dynamic_update_index_in_dim(whole, block, (chip - step) % chips, 0)
    return whole


def layer(
    layer_input,
    norm_gain,
    key_weight,
    value_weight,
    input_gate_weight,
    forget_gate_weight,
    conv_weight,
    input_shift,
    forget_shift,
    new_query,
    new_key,
    new_value,
    new_input,
    new_forget,
):
    _, rows, _ = layer_input.shape
    lines = rows // DK
    core = lax.axis_index("sp") % 2
    key_blocks, normed = project_keys(
        layer_input, norm_gain, key_weight, input_gate_weight, forget_gate_weight
    )
    kept, given = project_values(normed, value_weight, rows)
    value_blocks = trade(kept, given)
    mine = in_order(spread(rotate(key_blocks)))
    own = lax.dynamic_index_in_dim(mine, core, 1, keepdims=False)
    other = lax.dynamic_index_in_dim(mine, 1 - core, 1, keepdims=False)
    mine = trade(own, other).reshape((-1,) + own.shape[1:])
    values = spread(rotate(value_blocks))
    length = mine.shape[0] * rows
    key_linear = mine[:, :rows].reshape(length, DK)
    input_linear = mine[:, rows : rows + lines].reshape(1, 1, length)
    forget_linear = mine[:, rows + lines : rows + 2 * lines].reshape(1, 1, length)
    head = lax.axis_index("tp")
    tap_weight = lax.dynamic_slice(conv_weight, (0, head * DK), (CONV, DK))
    keys = convolve(key_linear, tap_weight).reshape(1, 1, length, DK)
    values, weight_cache, first_read = read_cache(
        keys,
        values,
        input_linear,
        forget_linear,
        input_shift,
        forget_shift,
        new_query,
        new_key,
        new_value,
        new_input,
        new_forget,
    )
    return (keys, values.reshape(keys.shape), weight_cache, first_read.reshape(new_value.shape))


def solution(mesh):
    in_specs = (
        P(("grp", "tp"), "sp", None),
        P(),
        P(),
        P(),
        P(),
        P(),
        P(),
        P(("grp", "sp"), "tp", None),
        P(("grp", "sp"), "tp", None),
        P(("grp", "sp"), "tp", None),
        P(("grp", "sp"), "tp", None),
        P(("grp", "sp"), "tp", None),
        P(("grp", "sp"), "tp"),
        P(("grp", "sp"), "tp"),
    )
    out_specs = (
        P(("grp", "sp"), "tp", None, None),
        P(("grp", "sp"), "tp", None, None),
        P(("grp", "sp"), "tp", None),
        P(("grp", "sp"), "tp", None),
    )
    return jax.shard_map(layer, mesh=mesh, in_specs=in_specs, out_specs=out_specs, check_vma=False)
```
